32 devices in a mesh: grp: 2 (over x), ep: 16 (over z, y, core).
Axes of the slice: x: 2, y: 2, z: 4, core: 2. Of those that a mesh axis runs over, the one named last changes fastest.
Arguments:
- tokens: bfloat16 [128, 2048], P(('grp', 'ep')), parts along dimension 0, may hold values from -30 to 30
- state: float32 [128, 16, 128, 128], P(('grp', 'ep')), parts along dimension 0, may hold values from -6 to 6
- route_ids: int32 [128, 2], P(('grp', 'ep')), parts along dimension 0, may hold values from 0 to 3, all different within a row; in each aligned block of 4 rows (0 to 3, 4 to 7, ...) at most 3 rows name the same one
- route_weights: bfloat16 [128, 2], P(('grp', 'ep')), parts along dimension 0, may hold values from 0.099609375 to 1
- norm_mix: float32 [2048], replicated, may hold values from 0.1 to 1.9
- w_query: bfloat16 [2048, 2048], P(None, 'ep'), may hold values from -0.125 to 0.125
- w_forget: bfloat16 [2048, 2048], P(None, 'ep'), may hold values from -0.125 to 0.125
- w_input: bfloat16 [2048, 2048], P(None, 'ep'), may hold values from -0.125 to 0.125
- w_gate: bfloat16 [2048, 2048], P(None, 'ep'), may hold values from -0.125 to 0.125
- lower_bound: float32 [2048], replicated, may hold values from 0.05 to 0.9
- head_gain: float32 [128], replicated, may hold values from 0.1 to 1.9
- w_out: bfloat16 [2048, 2048], P(None, 'ep'), may hold values from -0.125 to 0.125
- norm_ffn: float32 [2048], replicated, may hold values from 0.1 to 1.9
- expert_gate: bfloat16 [2048, 28672], P(None, 'ep'), may hold values from -0.125 to 0.125
- expert_up: bfloat16 [2048, 28672], P(None, 'ep'), may hold values from -0.125 to 0.125
- expert_down: bfloat16 [28672, 2048], P('ep'), may hold values from -0.0625 to 0.0625
Outputs:
- layer_out: bfloat16 [128, 2048], P(('grp', 'ep')), parts along dimension 0
- new_state: float32 [128, 16, 128, 128], P(('grp', 'ep')), parts along dimension 0
The draws below stay inside these ranges and needn't reach their ends.
There are 2 independent parts, one for each index of `grp`. The reference program is written for one: setup_inputs(seed, part) draws one part's arguments, and reference() takes and returns one part's arrays. A program takes and returns all parts, laid end to end along the dimension named above; an argument that names none is the same for every part. Nothing has to cross between parts.
Inputs may be any that keep to these rules, and one draw needn't show every extreme that they name: `route_ids`: each row names 2 different experts; the rows of one device name no expert more than 3 times, and some device names one exactly 3 times.
All inputs are finite; a program needn't handle non-finite values.
Results may differ from the reference program's by a relative error of at most 0.008.
Values may be sent and summed in bfloat16 or wider, within the bound.
A program may use at most 64 MiB of HBM per device.

```python
import math
import jax
import jax.numpy as jnp
import numpy as np
from jax import lax

D = 2048
HEAD_DIM = 128
HEADS = 16
FF = 7168
EXPERTS = 4
TOP_K = 2
SEQ_DEV = 4
TOKENS = 64
CAP = 3


def draw_tokens(key, part):
    row_key, col_key, value_key = jax.random.split(key, 3)
    col_scale = jnp.exp(jnp.linspace(jnp.log(0.3), jnp.log(3.0), D))
    col_scale = col_scale * jnp.exp(jax.random.uniform(col_key, (D,), jnp.float32, -0.35, 0.35))
    row_scale = jnp.exp(jax.random.uniform(row_key, (TOKENS, 1), jnp.float32, jnp.log(0.5), jnp.log(1.5)))
    values = jax.random.normal(value_key, (TOKENS, D), jnp.float32)
    return jnp.clip(values * row_scale * col_scale[None, :], -30.0, 30.0).astype(jnp.bfloat16)


def block_scale(own_key, shape, cuts, low, top_value):
    factor_of, own = 1.0, jax.random.fold_in(own_key, 6)
    for position, shards_of in cuts:
        steps = jnp.exp(jax.random.uniform(jax.random.fold_in(own, position), (shards_of,), jnp.float32, low / len(cuts), top_value / len(cuts)))
        factor_of = factor_of * jnp.repeat(steps, shape[position] // shards_of).reshape([-1 if axis == position else 1 for axis in range(len(shape))])
    return factor_of


def assign_block(rng, own, number, rows, count, top, most, skew):
    ranking = jax.random.permutation(rng, count)
    heavy_load, ordinary = load_shares(count, rows * top, most, skew, True), load_shares(count, rows * top, most, skew, False)
    places = jnp.arange(count)

    def named(tallies, offset_by):
        used = int((tallies > 0).sum())
        fixed = max(1, used // 4)
        shifted = fixed + (places - fixed + offset_by * (used - fixed)) % max(1, count - fixed)
        return jnp.zeros((count,), jnp.int32).at[ranking[jnp.where(places < fixed, places, shifted)]].set(jnp.asarray(tallies, jnp.int32))

    tallies = jnp.where(number % 4 == 0, named(heavy_load, number // 4), named(ordinary, number - number // 4 - 1))
    mixed = jax.random.permutation(jax.random.fold_in(own, 3), count)
    giver, receiver = mixed[0:count // 2 * 2:2], mixed[1:count // 2 * 2:2]
    slack = jnp.minimum(tallies[giver] - 1, most - tallies[receiver]) // 2
    slack = jnp.where((giver == ranking[0]) | (receiver == ranking[0]) | (tallies[receiver] == 0), 0, jnp.maximum(slack, 0))
    shifted = jax.random.randint(jax.random.fold_in(own, 4), (count // 2,), 0, 1 << 20) % (slack + 1)
    tallies = tallies.at[giver].add(-shifted).at[receiver].add(shifted)
    members = jnp.searchsorted(jnp.cumsum(tallies), jnp.arange(rows * top), side="right").astype(jnp.int32)
    grid = members.reshape(top, rows).T
    grid = grid[jax.random.permutation(jax.random.fold_in(own, 1), rows)]
    offset_by = jax.random.randint(jax.random.fold_in(own, 2), (rows, 1), 0, top)
    return jnp.take_along_axis(grid, (jnp.arange(top)[None, :] + offset_by) % top, axis=1)


def load_shares(amount, total, limit, lean, full):
    weights = [(1 << 20) // math.isqrt(rank ** lean) + 1 for rank in range(1, amount + 1)]
    largest = limit if full else min(limit, max(-(-total // amount), total * weights[0] // sum(weights)))
    least = 1 if total - largest >= amount - 1 else 0
    given, spare = [largest] + [least] * (amount - 1), total - largest - least * (amount - 1)
    while spare > 0:
        movable = [i for i in range(1, amount) if given[i] < largest] or [i for i in range(1, amount) if given[i] < limit]
        pool, left = sum([weights[i] for i in movable]), spare
        for i in movable:
            extra = min(limit - given[i], max(1, left * weights[i] // pool), spare)
            given[i] = given[i] + extra
            spare = spare - extra
    return np.array(given)


def centred(own_key, dims, spread, bound, pieces=(), held_as=jnp.bfloat16):
    factor_of = block_scale(own_key, dims, pieces, -0.22, 0.18) if pieces else 1.0
    result = jax.random.normal(own_key, dims, jnp.float32) * spread * factor_of
    return jnp.minimum(jnp.maximum(result, -bound), bound).astype(held_as)


def setup_inputs(seed: int = 0, part: int = 0) -> dict:
    splits = jax.random.split(jax.random.key(seed), 17)
    part_keys = jax.random.split(jax.random.fold_in(splits[16], part), 17)
    tokens = draw_tokens(jax.random.fold_in(jax.random.fold_in(splits[16], part), 71), part)
    state = centred(part_keys[1], (TOKENS, HEADS, HEAD_DIM, HEAD_DIM), 1.0, 6.0, ((0, 16),), jnp.float32)
    route_ids_keys = jax.random.split(jax.random.fold_in(part_keys[2], 1), TOKENS // SEQ_DEV)
    route_ids_turns = jax.random.permutation(jax.random.fold_in(part_keys[2], 3), TOKENS // SEQ_DEV)
    route_ids = jax.vmap(lambda own, number: assign_block(jax.random.fold_in(part_keys[2], 2), own, number, SEQ_DEV, EXPERTS, TOP_K, CAP, 1))(route_ids_keys, route_ids_turns).reshape((TOKENS, TOP_K))
    route_weights = jnp.clip(0.099609375 + 0.9003906 * jax.random.uniform(part_keys[3], (TOKENS, TOP_K), jnp.float32) ** block_scale(part_keys[3], (TOKENS, TOP_K), ((0, 16),), -0.2, 0.2), 0.099609375, 1.0).astype(jnp.bfloat16)
    norm_mix = jnp.clip(1.0 + 0.18 * jax.random.normal(splits[4], (D,), jnp.float32), 0.1, 1.9)
    w_query = centred(splits[5], (D, D), D ** -0.5, 0.125, ((1, 16),))
    w_forget = centred(splits[6], (D, D), D ** -0.5, 0.125, ((1, 16),))
    w_input = centred(splits[7], (D, D), D ** -0.5, 0.125, ((1, 16),))
    w_gate = centred(splits[8], (D, D), D ** -0.5, 0.125, ((1, 16),))
    lower_bound = jnp.clip(jax.random.uniform(splits[9], (D,), jnp.float32, 0.05, 0.9), 0.05, 0.9)
    head_gain = jnp.clip(1.0 + 0.18 * jax.random.normal(splits[10], (HEAD_DIM,), jnp.float32), 0.1, 1.9)
    w_out = centred(splits[11], (D, D), D ** -0.5, 0.125, ((1, 16),))
    norm_ffn = jnp.clip(1.0 + 0.18 * jax.random.normal(splits[12], (D,), jnp.float32), 0.1, 1.9)
    expert_gate = centred(splits[13], (D, EXPERTS * FF), D ** -0.5, 0.125, ((1, 16),))
    expert_up = centred(splits[14], (D, EXPERTS * FF), D ** -0.5, 0.125, ((1, 16),))
    expert_down = centred(splits[15], (EXPERTS * FF, D), FF ** -0.5, 0.0625, ((0, 16),))
    return dict(tokens=tokens, state=state, route_ids=route_ids, route_weights=route_weights, norm_mix=norm_mix, w_query=w_query, w_forget=w_forget, w_input=w_input, w_gate=w_gate, lower_bound=lower_bound, head_gain=head_gain, w_out=w_out, norm_ffn=norm_ffn, expert_gate=expert_gate, expert_up=expert_up, expert_down=expert_down)


epsilon = 1e-06

def rms_scale(values, gain):
    return values * lax.rsqrt(lax.optimization_barrier(jnp.mean(values * values, axis=-1, keepdims=True)) + epsilon) * gain

def mixer_state(projected, state, lower_bound, head_gain):
    query_raw = projected[0].astype(jnp.float32)
    forget_raw = projected[1].astype(jnp.float32)
    input_raw = projected[2].astype(jnp.float32)
    gate_raw = projected[3].astype(jnp.float32)
    seq_rows = state.shape[0]
    heads = state.shape[1]
    head_dim = state.shape[2]
    head_shape = (seq_rows, heads, head_dim)
    floor_rate = lower_bound.astype(jnp.float32)
    log_forget = jnp.logaddexp(jnp.log(floor_rate), jnp.log1p(-floor_rate) + jax.nn.log_sigmoid(forget_raw))
    key_vec = (1.0 - floor_rate) * jax.nn.sigmoid(-forget_raw)
    query_vec = jax.nn.silu(query_raw) * head_dim ** (-0.5)
    new_state = jnp.exp(log_forget).reshape(head_shape)[..., None] * state + key_vec.reshape(head_shape)[..., None] * input_raw.reshape(head_shape)[:, :, None, :]
    read_out = jnp.einsum('thk,thkv->thv', query_vec.reshape(head_shape), new_state, precision=lax.Precision.HIGHEST)
    mixed = rms_scale(read_out, head_gain) * jax.nn.silu(gate_raw.reshape(head_shape))
    return (mixed.reshape(seq_rows, heads * head_dim).astype(jnp.bfloat16), new_state)

def reference(tokens, state, route_ids, route_weights, norm_mix, w_query, w_forget, w_input, w_gate, lower_bound, head_gain, w_out, norm_ffn, expert_gate, expert_up, expert_down):
    resid = tokens.astype(jnp.float32)
    normed = rms_scale(resid, norm_mix).astype(jnp.bfloat16)
    projected = jnp.stack([jnp.dot(normed, weight, preferred_element_type=jnp.float32).astype(jnp.bfloat16) for weight in (w_query, w_forget, w_input, w_gate)])
    mixed, new_state = mixer_state(projected, state, lower_bound, head_gain)
    mixer_out = jnp.dot(mixed, w_out, preferred_element_type=jnp.float32).astype(jnp.bfloat16)
    middle = resid + mixer_out.astype(jnp.float32)
    normed_two = rms_scale(middle, norm_ffn).astype(jnp.bfloat16)
    matches = (route_ids[:, :, None] == jnp.arange(EXPERTS, dtype=jnp.int32)[None, None, :]).astype(jnp.float32)
    combined = lax.optimization_barrier(jnp.sum(route_weights.astype(jnp.float32)[:, :, None] * matches, axis=1))
    expert_total = jnp.zeros_like(middle)
    for expert in range(EXPERTS):
        gate_act = jnp.dot(normed_two, expert_gate[:, expert * FF:(expert + 1) * FF], preferred_element_type=jnp.float32)
        up_act = jnp.dot(normed_two, expert_up[:, expert * FF:(expert + 1) * FF], preferred_element_type=jnp.float32)
        hidden = (jax.nn.silu(gate_act) * up_act).astype(jnp.bfloat16)
        down_act = jnp.dot(hidden, expert_down[expert * FF:(expert + 1) * FF, :], preferred_element_type=jnp.float32)
        expert_total = expert_total + combined[:, expert:expert + 1] * down_act
    return ((middle + expert_total).astype(jnp.bfloat16), new_state)
```

```python
import functools

import jax
import jax.numpy as jnp
from jax import lax
from jax.experimental import pallas as pl
from jax.experimental.pallas import tpu as pltpu
from jax.sharding import PartitionSpec as P

FF = 7168
EXPERTS = 4

epsilon = 1e-06
F32 = jnp.float32
BF16 = jnp.bfloat16


def rms_scale(values, gain):
    return values * lax.rsqrt(jnp.mean(values * values, axis=-1, keepdims=True) + epsilon) * gain


def kernel(
    n,
    tokens,
    state,
    ids,
    weights,
    norm_mix,
    w_query,
    w_forget,
    w_input,
    w_gate,
    lower_bound,
    head_gain,
    w_out,
    norm_ffn,
    expert_gate,
    expert_up,
    expert_down,
    layer_out,
    new_state,
    tok_buf,
    st,
    wp,
    wo,
    wg,
    wu,
    wd,
    xn,
    pj_send,
    pj_buf,
    gates,
    reads,
    mx_buf,
    col_buf,
    mid_buf,
    hid,
    ps,
    ret_buf,
    load_sem,
    store_sem,
    send_sem,
    recv_sem,
):
    me = lax.axis_index("ep")
    rows, width = tokens.shape
    heads, dim = state.shape[1], state.shape[2]
    cols = w_query.shape[1]
    total = n * rows
    hidden = expert_gate.shape[1]
    group = n // EXPERTS
    chunk = 16
    per = chunk // rows

    loads = [pltpu.make_async_copy(tokens, tok_buf.at[me], load_sem.at[0])]
    for j, w in enumerate((w_query, w_forget, w_input, w_gate)):
        loads.append(pltpu.make_async_copy(w, wp.at[j], load_sem.at[1 + j]))
    loads.append(pltpu.make_async_copy(state, st, load_sem.at[5]))
    loads.append(pltpu.make_async_copy(w_out, wo, load_sem.at[6]))
    loads.append(pltpu.make_async_copy(expert_gate, wg, load_sem.at[7]))
    loads.append(pltpu.make_async_copy(expert_up, wu, load_sem.at[8]))
    loads.append(pltpu.make_async_copy(expert_down, wd, load_sem.at[9]))

    barrier = pltpu.get_barrier_semaphore()
    for k in range(1, n):
        pl.semaphore_signal(
            barrier,
            inc=1,
            device_id={"ep": lax.rem(me + k, n)},
            device_id_type=pl.DeviceIdType.MESH,
        )
    for load in loads:
        load.start()
    pl.semaphore_wait(barrier, n - 1)

    def exchange(phase, source, target):
        copies = []
        for k in range(1, n):
            peer = lax.rem(me + k, n)
            copy = pltpu.make_async_remote_copy(
                src_ref=source(peer),
                dst_ref=target.at[me],
                send_sem=send_sem.at[phase, k],
                recv_sem=recv_sem.at[phase, k],
                device_id={"ep": peer},
                device_id_type=pl.DeviceIdType.MESH,
            )
            copy.start()
            copies.append(copy)
        return copies

    def arrive(copies):
        for copy in copies:
            copy.wait_recv()

    loads[0].wait()
    sent = [exchange(0, lambda peer: tok_buf.at[me], tok_buf)]
    arrive(sent[0])

    def norm_chunk(c, carry):
        x = jnp.concatenate([tok_buf[c * per + i].astype(F32) for i in range(per)], axis=0)
        r0 = pl.multiple_of(c * chunk, chunk)
        xn[pl.ds(r0, chunk), :] = rms_scale(x, norm_mix[...]).astype(BF16)
        return carry

    lax.fori_loop(0, total // chunk, norm_chunk, 0)

    for load in loads[1:5]:
        load.wait()
    w_all = jnp.concatenate([wp[j] for j in range(4)], axis=1)
    acc = jnp.dot(xn[...], w_all, preferred_element_type=F32)
    for s in range(n):
        pj_send[s] = acc[s * rows : (s + 1) * rows, :].astype(BF16)
    sent.append(exchange(1, lambda peer: pj_send.at[peer], pj_buf))
    pj_buf[me] = pj_send[me]
    loads[5].wait()
    arrive(sent[1])

    def owned(j):
        return jnp.concatenate(
            [pj_buf[s][:, j * cols : (j + 1) * cols].astype(F32) for s in range(n)], axis=1
        )

    bound = lower_bound[...]
    forget_raw = owned(1)
    query_raw = owned(0)
    decay = bound + (1.0 - bound) * jax.nn.sigmoid(forget_raw)
    key_vec = (1.0 - bound) * jax.nn.sigmoid(-forget_raw)
    query_vec = jax.nn.silu(query_raw) * dim ** (-0.5)
    input_raw = owned(2)
    for h in range(heads):
        part = slice(h * dim, (h + 1) * dim)
        gates[h] = jnp.concatenate(
            [decay[:, part], key_vec[:, part], query_vec[:, part], input_raw[:, part]], axis=0
        )

    def head_step(h, carry):
        flat = gates[h]
        turned = flat.T
        out = []
        for t in range(rows):
            fresh = (
                turned[:, t : t + 1] * st[t, h]
                + turned[:, rows + t : rows + t + 1] * flat[3 * rows + t : 3 * rows + t + 1, :]
            )
            st[t, h] = fresh
            out.append(
                jnp.sum(turned[:, 2 * rows + t : 2 * rows + t + 1] * fresh, axis=0, keepdims=True)
            )
        reads[h] = jnp.concatenate(out, axis=0)
        return carry

    lax.fori_loop(0, heads, head_step, 0)

    gate_raw = owned(3)
    mixed = jnp.concatenate(
        [
            rms_scale(reads[h], head_gain[...]) * jax.nn.silu(gate_raw[:, h * dim : (h + 1) * dim])
            for h in range(heads)
        ],
        axis=1,
    )
    mx_buf[me] = mixed.astype(BF16)

    sent.append(exchange(2, lambda peer: mx_buf.at[me], mx_buf))
    keep = pltpu.make_async_copy(st, new_state, store_sem)
    keep.start()
    loads[6].wait()
    arrive(sent[2])

    def mixed_chunk(c, carry):
        x = jnp.concatenate([mx_buf[c * per + i].astype(F32) for i in range(per)], axis=0)
        r0 = pl.multiple_of(c * chunk, chunk)
        xn[pl.ds(r0, chunk), :] = x.astype(BF16)
        return carry

    lax.fori_loop(0, total // chunk, mixed_chunk, 0)
    col_buf[me] = jnp.dot(xn[...], wo[...], preferred_element_type=F32).astype(BF16)

    sent.append(exchange(3, lambda peer: col_buf.at[me], col_buf))
    arrive(sent[3])

    def middle_chunk(c, carry):
        r0 = pl.multiple_of(c * chunk, chunk)
        x = jnp.concatenate([tok_buf[c * per + i].astype(F32) for i in range(per)], axis=0)
        y = jnp.concatenate(
            [col_buf[s, pl.ds(r0, chunk), :].astype(F32) for s in range(n)], axis=1
        )
        middle = x + y
        for i in range(per):
            mid_buf[c * per + i] = middle[i * rows : (i + 1) * rows, :]
        xn[pl.ds(r0, chunk), :] = rms_scale(middle, norm_ffn[...]).astype(BF16)
        return carry

    lax.fori_loop(0, total // chunk, middle_chunk, 0)

    loads[7].wait()
    loads[8].wait()
    tile = 256 if hidden % 256 == 0 else hidden

    def up_tile(j, carry):
        part = pl.ds(pl.multiple_of(j * tile, tile) if tile % 128 == 0 else 0, tile)
        g = jnp.dot(xn[...], wg[:, part], preferred_element_type=F32)
        u = jnp.dot(xn[...], wu[:, part], preferred_element_type=F32)
        hid[:, part] = (jax.nn.silu(g) * u).astype(BF16)
        return carry

    lax.fori_loop(0, hidden // tile, up_tile, 0)
    loads[9].wait()
    out_tile = 256

    def down_tile(j, carry):
        part = pl.ds(pl.multiple_of(j * out_tile, out_tile), out_tile)
        d = jnp.dot(hid[...], wd[:, part], preferred_element_type=F32)
        for s in range(n):
            ps[s, :, part] = d[s * rows : (s + 1) * rows, :].astype(BF16)
        return carry

    lax.fori_loop(0, width // out_tile, down_tile, 0)

    sent.append(exchange(4, lambda peer: ps.at[peer], ret_buf))
    ret_buf[me] = ps[me]
    arrive(sent[4])
    result = mid_buf[me]
    for e in range(EXPERTS):
        share = jnp.sum(
            jnp.where(ids[...] == e, weights[...].astype(F32), 0.0), axis=1, keepdims=True
        )
        rows_e = ret_buf[e * group].astype(F32)
        for s in range(1, group):
            rows_e = rows_e + ret_buf[e * group + s].astype(F32)
        result = result + share * rows_e
    layer_out[...] = result.astype(BF16)

    for copies in sent:
        for copy in copies:
            copy.wait_send()
    keep.wait()


def local(n, *args):
    (
        tokens,
        state,
        ids,
        weights,
        norm_mix,
        w_query,
        w_forget,
        w_input,
        w_gate,
        lower_bound,
        head_gain,
        w_out,
        norm_ffn,
        expert_gate,
        expert_up,
        expert_down,
    ) = args
    rows, width = tokens.shape
    heads, dim = state.shape[1], state.shape[2]
    cols = w_query.shape[1]
    hidden = expert_gate.shape[1]
    total = n * rows
    any_spec = pl.BlockSpec(memory_space=pl.ANY)
    vmem = pl.BlockSpec(memory_space=pltpu.VMEM)
    return pl.pallas_call(
        functools.partial(kernel, n),
        out_shape=(
            jax.ShapeDtypeStruct(tokens.shape, tokens.dtype),
            jax.ShapeDtypeStruct(state.shape, state.dtype),
        ),
        in_specs=[any_spec, any_spec, vmem, vmem, vmem]
        + [any_spec] * 4
        + [vmem, vmem, any_spec, vmem]
        + [any_spec] * 3,
        out_specs=(vmem, any_spec),
        scratch_shapes=[
            pltpu.VMEM((n, rows, width), BF16),
            pltpu.VMEM(state.shape, F32),
            pltpu.VMEM((4, width, cols), BF16),
            pltpu.VMEM((width, cols), BF16),
            pltpu.VMEM((width, hidden), BF16),
            pltpu.VMEM((width, hidden), BF16),
            pltpu.VMEM((hidden, width), BF16),
            pltpu.VMEM((total, width), BF16),
            pltpu.VMEM((n, rows, 4 * cols), BF16),
            pltpu.VMEM((n, rows, 4 * cols), BF16),
            pltpu.VMEM((heads, 4 * rows, dim), F32),
            pltpu.VMEM((heads, rows, dim), F32),
            pltpu.VMEM((n, rows, width), BF16),
            pltpu.VMEM((n, total, cols), BF16),
            pltpu.VMEM((n, rows, width), F32),
            pltpu.VMEM((total, hidden), BF16),
            pltpu.VMEM((n, rows, width), BF16),
            pltpu.VMEM((n, rows, width), BF16),
            pltpu.SemaphoreType.DMA((10,)),
            pltpu.SemaphoreType.DMA,
            pltpu.SemaphoreType.DMA((5, n)),
            pltpu.SemaphoreType.DMA((5, n)),
        ],
        compiler_params=pltpu.CompilerParams(collective_id=0, has_side_effects=True),
    )(
        tokens,
        state,
        ids,
        weights,
        norm_mix[None],
        w_query,
        w_forget,
        w_input,
        w_gate,
        lower_bound[None],
        head_gain[None],
        w_out,
        norm_ffn[None],
        expert_gate,
        expert_up,
        expert_down,
    )


def solution(mesh):
    return jax.shard_map(
        functools.partial(local, mesh.shape["ep"]),
        mesh=mesh,
        in_specs=(
            P(("grp", "ep"), None),
            P(("grp", "ep"), None, None, None),
            P(("grp", "ep"), None),
            P(("grp", "ep"), None),
            P(),
            P(None, "ep"),
            P(None, "ep"),
            P(None, "ep"),
            P(None, "ep"),
            P(),
            P(),
            P(None, "ep"),
            P(),
            P(None, "ep"),
            P(None, "ep"),
            P("ep", None),
        ),
        out_specs=(P(("grp", "ep"), None), P(("grp", "ep"), None, None, None)),
        check_vma=False,
    )
```

```python
import functools

import jax
import jax.numpy as jnp
from jax import lax
from jax.experimental import pallas as pl
from jax.experimental.pallas import tpu as pltpu
from jax.sharding import PartitionSpec as P

FF = 7168
EXPERTS = 4
VMEM = 67043328

epsilon = 1e-06
F32 = jnp.float32
BF16 = jnp.bfloat16


def rms_scale(values, gain):
    return values * lax.rsqrt(jnp.mean(values * values, axis=-1, keepdims=True) + epsilon) * gain


def kernel(
    n,
    tokens,
    state,
    ids,
    weights,
    norm_mix_in,
    w_query,
    w_forget,
    w_input,
    w_gate,
    lower_bound_in,
    head_gain_in,
    w_out,
    norm_ffn_in,
    expert_gate,
    expert_up,
    expert_down,
    layer_out,
    st,
    tok_buf,
    norm_mix,
    lower_bound,
    head_gain,
    norm_ffn,
    wp,
    wo,
    wg,
    wu,
    wd,
    xn,
    pj_send,
    pj_buf,
    gates,
    reads,
    mx_buf,
    col_buf,
    mid_buf,
    hid,
    ps,
    fw,
    summed,
    ret_buf,
    load_sem,
    send_sem,
    recv_sem,
):
    me = lax.axis_index("ep")
    rows, width = tokens.shape
    heads, dim = state.shape[1], state.shape[2]
    cols = w_query.shape[1]
    total = n * rows
    hidden = expert_gate.shape[1]
    group = n // EXPERTS // 2
    chunk = 16
    per = chunk // rows

    loads = [pltpu.make_async_copy(tokens, tok_buf.at[me], load_sem.at[0])]
    for j, w in enumerate((w_query, w_forget, w_input, w_gate)):
        loads.append(pltpu.make_async_copy(w, wp.at[j], load_sem.at[1 + j]))
    loads.append(pltpu.make_async_copy(state, st, load_sem.at[5]))
    loads.append(pltpu.make_async_copy(w_out, wo, load_sem.at[6]))
    loads.append(pltpu.make_async_copy(expert_gate, wg, load_sem.at[7]))
    loads.append(pltpu.make_async_copy(expert_up, wu, load_sem.at[8]))
    loads.append(pltpu.make_async_copy(expert_down, wd, load_sem.at[9]))
    small = [
        pltpu.make_async_copy(a, b, load_sem.at[10 + j])
        for j, (a, b) in enumerate(
            (
                (norm_mix_in, norm_mix),
                (lower_bound_in, lower_bound),
                (head_gain_in, head_gain),
                (norm_ffn_in, norm_ffn),
            )
        )
    ]

    core = lax.rem(me, 2)
    chip = me // 2
    chips = n // 2
    partner = me + 1 - 2 * core
    others = []
    for k in range(1, chips // 2 + 1):
        others.extend(sorted({k, chips - k}))

    def away(k):
        return lax.rem(me + 2 * k, n)

    barrier = pltpu.get_barrier_semaphore()
    for k in range(1, n):
        pl.semaphore_signal(
            barrier,
            inc=1,
            device_id={"ep": lax.rem(me + k, n)},
            device_id_type=pl.DeviceIdType.MESH,
        )
    for load in loads[:1] + small + loads[1:]:
        load.start()
    pl.semaphore_wait(barrier, n - 1)
    sent = []

    def send(phase, slot, source, target, peer):
        copy = pltpu.make_async_remote_copy(
            src_ref=source,
            dst_ref=target,
            send_sem=send_sem.at[phase, slot],
            recv_sem=recv_sem.at[phase, slot],
            device_id={"ep": peer},
            device_id_type=pl.DeviceIdType.MESH,
        )
        copy.start()
        sent.append(copy)
        return copy

    def spread(phase, buf):
        block = buf.at[me]
        direct = {k: send(phase, k, block, block, away(k)) for k in others}
        passed = [send(phase, chips, block, block, partner)]
        return direct, passed

    def pass_on(phase, buf, copies):
        direct, passed = copies
        for k in others:
            direct[k].wait_recv()
            block = buf.at[lax.rem(me - 2 * k + n, n)]
            passed.append(send(phase, chips + k, block, block, partner))
        for copy in passed:
            copy.wait_recv()

    loads[0].wait()
    copies = spread(0, tok_buf)
    for load in small:
        load.wait()
    pass_on(0, tok_buf, copies)

    def norm_chunk(c, carry):
        x = jnp.concatenate([tok_buf[c * per + i].astype(F32) for i in range(per)], axis=0)
        r0 = pl.multiple_of(c * chunk, chunk)
        xn[pl.ds(r0, chunk), :] = rms_scale(x, norm_mix[...]).astype(BF16)
        return carry

    lax.fori_loop(0, total // chunk, norm_chunk, 0)

    for load in loads[1:5]:
        load.wait()
    w_all = jnp.concatenate([wp[j] for j in range(4)], axis=1)
    acc = jnp.dot(xn[...], w_all, preferred_element_type=F32)
    for s in range(n):
        pj_send[s] = acc[s * rows : (s + 1) * rows, :].astype(BF16)
    copies = [
        send(1, k, pj_send.at[lax.rem(me + k, n)], pj_buf.at[me], lax.rem(me + k, n))
        for k in range(1, n)
    ]
    pj_buf[me] = pj_send[me]
    loads[5].wait()
    for copy in copies:
        copy.wait_recv()

    def owned(j):
        return jnp.concatenate(
            [pj_buf[s][:, j * cols : (j + 1) * cols].astype(F32) for s in range(n)], axis=1
        )

    bound = lower_bound[...]
    forget_raw = owned(1)
    query_raw = owned(0)
    decay = bound + (1.0 - bound) * jax.nn.sigmoid(forget_raw)
    key_vec = (1.0 - bound) * jax.nn.sigmoid(-forget_raw)
    query_vec = jax.nn.silu(query_raw) * dim ** (-0.5)
    input_raw = owned(2)
    read_vec = query_vec * decay
    for h in range(heads):
        part = slice(h * dim, (h + 1) * dim)
        gates[h] = jnp.concatenate(
            [read_vec[:, part], decay[:, part], key_vec[:, part], input_raw[:, part]], axis=0
        )

    def read_step(h, carry):
        turned = gates[h].T
        out = [
            jnp.sum(turned[:, t : t + 1] * st[t, h], axis=0, keepdims=True) for t in range(rows)
        ]
        reads[h] = jnp.concatenate(out, axis=0)
        return carry

    lax.fori_loop(0, heads, read_step, 0, unroll=4)

    def update_step(h, carry):
        flat = gates[h]
        turned = flat.T
        for t in range(rows):
            st[t, h] = (
                turned[:, rows + t : rows + t + 1] * st[t, h]
                + turned[:, 2 * rows + t : 2 * rows + t + 1]
                * flat[3 * rows + t : 3 * rows + t + 1, :]
            )
        return carry

    gate_raw = owned(3)
    query_key = query_vec * key_vec
    mixed = jnp.concatenate(
        [
            rms_scale(
                reads[h]
                + jnp.sum(query_key[:, h * dim : (h + 1) * dim], axis=1, keepdims=True)
                * input_raw[:, h * dim : (h + 1) * dim],
                head_gain[...],
            )
            * jax.nn.silu(gate_raw[:, h * dim : (h + 1) * dim])
            for h in range(heads)
        ],
        axis=1,
    )
    mx_buf[me] = mixed.astype(BF16)

    copies = spread(2, mx_buf)
    lax.fori_loop(0, heads // 2, update_step, 0, unroll=2)
    loads[6].wait()
    pass_on(2, mx_buf, copies)

    def mixed_chunk(c, carry):
        x = jnp.concatenate([mx_buf[c * per + i].astype(F32) for i in range(per)], axis=0)
        r0 = pl.multiple_of(c * chunk, chunk)
        xn[pl.ds(r0, chunk), :] = x.astype(BF16)
        return carry

    lax.fori_loop(0, total // chunk, mixed_chunk, 0)
    col_buf[me] = jnp.dot(xn[...], wo[...], preferred_element_type=F32).astype(BF16)

    copies = spread(3, col_buf)
    lax.fori_loop(heads // 2, heads, update_step, 0, unroll=2)
    pass_on(3, col_buf, copies)

    def middle_chunk(c, carry):
        r0 = pl.multiple_of(c * chunk, chunk)
        x = jnp.concatenate([tok_buf[c * per + i].astype(F32) for i in range(per)], axis=0)
        y = jnp.concatenate(
            [col_buf[s, pl.ds(r0, chunk), :].astype(F32) for s in range(n)], axis=1
        )
        middle = x + y
        for i in range(per):
            mid_buf[c * per + i] = middle[i * rows : (i + 1) * rows, :]
        xn[pl.ds(r0, chunk), :] = rms_scale(middle, norm_ffn[...]).astype(BF16)
        return carry

    lax.fori_loop(0, total // chunk, middle_chunk, 0)

    loads[7].wait()
    loads[8].wait()
    tile = 256 if hidden % 256 == 0 else hidden

    def up_tile(j, carry):
        part = pl.ds(pl.multiple_of(j * tile, tile) if tile % 128 == 0 else 0, tile)
        g = jnp.dot(xn[...], wg[:, part], preferred_element_type=F32)
        u = jnp.dot(xn[...], wu[:, part], preferred_element_type=F32)
        hid[:, part] = (jax.nn.silu(g) * u).astype(BF16)
        return carry

    lax.fori_loop(0, hidden // tile, up_tile, 0)
    loads[9].wait()
    out_tile = 256
    pieces = 2
    piece = width // pieces

    def down_tile(j, carry):
        part = pl.ds(pl.multiple_of(j * out_tile, out_tile), out_tile)
        d = jnp.dot(hid[...], wd[:, part], preferred_element_type=F32)
        for s in range(n):
            ps[s % 2, s // 2, :, part] = d[s * rows : (s + 1) * rows, :].astype(BF16)
        return carry

    per_piece = piece // out_tile
    halves = []
    for p in range(pieces):
        lax.fori_loop(p * per_piece, (p + 1) * per_piece, down_tile, 0)
        part = pl.ds(p * piece, piece)
        halves.append(
            send(4, p, ps.at[1 - core, :, :, part], fw.at[:, :, part], partner)
        )
    returns = []
    for p in range(pieces):
        part = pl.ds(p * piece, piece)
        halves[p].wait_recv()
        for c in range(chips):
            summed[c, :, part] = (
                ps[core, c, :, part].astype(F32) + fw[c, :, part].astype(F32)
            ).astype(BF16)
        for k in others:
            to = lax.rem(chip + k, chips)
            returns.append(
                send(
                    5 + p,
                    k,
                    summed.at[to, :, part],
                    ret_buf.at[chip, :, part],
                    away(k),
                )
            )
        ret_buf[chip, :, part] = summed[chip, :, part]
    for copy in returns:
        copy.wait_recv()
    result = mid_buf[me]
    diagonal = lax.broadcasted_iota(jnp.int32, (rows, rows), 0) == lax.broadcasted_iota(
        jnp.int32, (rows, rows), 1
    )
    for e in range(EXPERTS):
        flat_share = jnp.sum(
            jnp.where(ids[...] == e, weights[...].astype(F32), 0.0), axis=0, keepdims=True
        )
        share = jnp.sum(jnp.where(diagonal, flat_share, 0.0), axis=1, keepdims=True)
        rows_e = ret_buf[e * group].astype(F32)
        for s in range(1, group):
            rows_e = rows_e + ret_buf[e * group + s].astype(F32)
        result = result + share * rows_e
    layer_out[...] = result.astype(BF16)

    for copy in sent:
        copy.wait_send()


def local(n, *args):
    (
        tokens,
        state,
        ids,
        weights,
        norm_mix,
        w_query,
        w_forget,
        w_input,
        w_gate,
        lower_bound,
        head_gain,
        w_out,
        norm_ffn,
        expert_gate,
        expert_up,
        expert_down,
    ) = args
    rows, width = tokens.shape
    heads, dim = state.shape[1], state.shape[2]
    cols = w_query.shape[1]
    hidden = expert_gate.shape[1]
    total = n * rows
    any_spec = pl.BlockSpec(memory_space=pltpu.HBM)
    vmem = pl.BlockSpec(memory_space=pltpu.VMEM)
    return pl.pallas_call(
        functools.partial(kernel, n),
        out_shape=(
            pltpu.VMEM(tokens.shape, tokens.dtype),
            pltpu.VMEM(state.shape, state.dtype),
        ),
        in_specs=[any_spec, any_spec, vmem, vmem] + [any_spec] * 12,
        out_specs=(vmem, vmem),
        scratch_shapes=[
            pltpu.VMEM((n, rows, width), BF16),
            pltpu.VMEM((1, width), F32),
            pltpu.VMEM((1, width), F32),
            pltpu.VMEM((1, dim), F32),
            pltpu.VMEM((1, width), F32),
            pltpu.VMEM((4, width, cols), BF16),
            pltpu.VMEM((width, cols), BF16),
            pltpu.VMEM((width, hidden), BF16),
            pltpu.VMEM((width, hidden), BF16),
            pltpu.VMEM((hidden, width), BF16),
            pltpu.VMEM((total, width), BF16),
            pltpu.VMEM((n, rows, 4 * cols), BF16),
            pltpu.VMEM((n, rows, 4 * cols), BF16),
            pltpu.VMEM((heads, 4 * rows, dim), F32),
            pltpu.VMEM((heads, rows, dim), F32),
            pltpu.VMEM((n, rows, width), BF16),
            pltpu.VMEM((n, total, cols), BF16),
            pltpu.VMEM((n, rows, width), F32),
            pltpu.VMEM((total, hidden), BF16),
            pltpu.VMEM((2, n // 2, rows, width), BF16),
            pltpu.VMEM((n // 2, rows, width), BF16),
            pltpu.VMEM((n // 2, rows, width), BF16),
            pltpu.VMEM((n // 2, rows, width), BF16),
            pltpu.SemaphoreType.DMA((14,)),
            pltpu.SemaphoreType.DMA((7, n)),
            pltpu.SemaphoreType.DMA((7, n)),
        ],
        compiler_params=pltpu.CompilerParams(
            collective_id=0,
            has_side_effects=True,
            vmem_limit_bytes=VMEM - 4 * state.size - 64 * 1024,
        ),
    )(
        tokens,
        state,
        ids.T,
        weights.T,
        norm_mix[None],
        w_query,
        w_forget,
        w_input,
        w_gate,
        lower_bound[None],
        head_gain[None],
        w_out,
        norm_ffn[None],
        expert_gate,
        expert_up,
        expert_down,
    )


def solution(mesh):
    return jax.shard_map(
        functools.partial(local, mesh.shape["ep"]),
        mesh=mesh,
        in_specs=(
            P(("grp", "ep"), None),
            P(("grp", "ep"), None, None, None),
            P(("grp", "ep"), None),
            P(("grp", "ep"), None),
            P(),
            P(None, "ep"),
            P(None, "ep"),
            P(None, "ep"),
            P(None, "ep"),
            P(),
            P(),
            P(None, "ep"),
            P(),
            P(None, "ep"),
            P(None, "ep"),
            P("ep", None),
        ),
        out_specs=(P(("grp", "ep"), None), P(("grp", "ep"), None, None, None)),
        check_vma=False,
    )
```

```python
import functools

import jax
import jax.numpy as jnp
from jax import lax
from jax.experimental import pallas as pl
from jax.experimental.pallas import tpu as pltpu
from jax.sharding import PartitionSpec as P

FF = 7168
EXPERTS = 4
VMEM = 67043328

epsilon = 1e-06
F32 = jnp.float32
BF16 = jnp.bfloat16


def rms_scale(values, gain):
    return values * lax.rsqrt(jnp.mean(values * values, axis=-1, keepdims=True) + epsilon) * gain


def kernel(
    n,
    tokens,
    state,
    ids,
    weights,
    norm_mix_in,
    w_query,
    w_forget,
    w_input,
    w_gate,
    lower_bound_in,
    head_gain_in,
    w_out,
    norm_ffn_in,
    expert_gate,
    expert_up,
    expert_down,
    layer_out,
    st,
    tok_buf,
    norm_mix,
    lower_bound,
    head_gain,
    norm_ffn,
    wp,
    wo,
    wg,
    wu,
    wd,
    xn,
    pj_send,
    pj_buf,
    gates,
    reads,
    mx_buf,
    col_buf,
    mid_buf,
    hid,
    ps,
    fw,
    summed,
    ret_buf,
    load_sem,
    send_sem,
    recv_sem,
):
    me = lax.axis_index("ep")
    rows, width = tokens.shape
    heads, dim = state.shape[1], state.shape[2]
    cols = w_query.shape[1]
    total = n * rows
    hidden = expert_gate.shape[1]
    group = n // EXPERTS // 2
    chunk = 16
    per = chunk // rows

    loads = [pltpu.make_async_copy(tokens, tok_buf.at[me], load_sem.at[0])]
    for j, w in enumerate((w_query, w_forget, w_input, w_gate)):
        loads.append(pltpu.make_async_copy(w, wp.at[j], load_sem.at[1 + j]))
    loads.append(pltpu.make_async_copy(state, st, load_sem.at[5]))
    loads.append(pltpu.make_async_copy(w_out, wo, load_sem.at[6]))
    loads.append(pltpu.make_async_copy(expert_gate, wg, load_sem.at[7]))
    loads.append(pltpu.make_async_copy(expert_up, wu, load_sem.at[8]))
    loads.append(pltpu.make_async_copy(expert_down, wd, load_sem.at[9]))
    small = [
        pltpu.make_async_copy(a, b, load_sem.at[10 + j])
        for j, (a, b) in enumerate(
            (
                (norm_mix_in, norm_mix),
                (lower_bound_in, lower_bound),
                (head_gain_in, head_gain),
                (norm_ffn_in, norm_ffn),
            )
        )
    ]

    core = lax.rem(me, 2)
    chip = me // 2
    chips = n // 2
    partner = me + 1 - 2 * core
    others = []
    for k in range(1, chips // 2 + 1):
        others.extend(sorted({k, chips - k}))

    def away(k):
        return lax.rem(me + 2 * k, n)

    barrier = pltpu.get_barrier_semaphore()
    for k in range(1, n):
        pl.semaphore_signal(
            barrier,
            inc=1,
            device_id={"ep": lax.rem(me + k, n)},
            device_id_type=pl.DeviceIdType.MESH,
        )
    for load in loads[:1] + small + loads[1:]:
        load.start()
    pl.semaphore_wait(barrier, n - 1)
    sent = []

    def send(phase, slot, source, target, peer):
        copy = pltpu.make_async_remote_copy(
            src_ref=source,
            dst_ref=target,
            send_sem=send_sem.at[phase, slot],
            recv_sem=recv_sem.at[phase, slot],
            device_id={"ep": peer},
            device_id_type=pl.DeviceIdType.MESH,
        )
        copy.start()
        sent.append(copy)
        return copy

    def spread(phase, buf):
        block = buf.at[me]
        direct = {k: send(phase, k, block, block, away(k)) for k in others}
        passed = [send(phase, chips, block, block, partner)]
        return direct, passed

    def pass_on(phase, buf, copies):
        direct, passed = copies
        for k in others:
            direct[k].wait_recv()
            block = buf.at[lax.rem(me - 2 * k + n, n)]
            passed.append(send(phase, chips + k, block, block, partner))
        for copy in passed:
            copy.wait_recv()

    loads[0].wait()
    copies = spread(0, tok_buf)
    for load in small:
        load.wait()
    pass_on(0, tok_buf, copies)

    def norm_chunk(c, carry):
        x = jnp.concatenate([tok_buf[c * per + i].astype(F32) for i in range(per)], axis=0)
        r0 = pl.multiple_of(c * chunk, chunk)
        xn[pl.ds(r0, chunk), :] = rms_scale(x, norm_mix[...]).astype(BF16)
        return carry

    lax.fori_loop(0, total // chunk, norm_chunk, 0, unroll=2)

    for load in loads[1:5]:
        load.wait()
    w_all = jnp.concatenate([wp[j] for j in range(4)], axis=1)
    acc = jnp.dot(xn[...], w_all, preferred_element_type=F32)
    for s in range(n):
        pj_send[s] = acc[s * rows : (s + 1) * rows, :].astype(BF16)
    copies = [
        send(1, k, pj_send.at[lax.rem(me + k, n)], pj_buf.at[me], lax.rem(me + k, n))
        for k in sorted(range(1, n), key=lambda k: min(k, n - k))
    ]
    pj_buf[me] = pj_send[me]
    loads[5].wait()
    for copy in copies:
        copy.wait_recv()

    def owned(j):
        return jnp.concatenate(
            [pj_buf[s][:, j * cols : (j + 1) * cols].astype(F32) for s in range(n)], axis=1
        )

    bound = lower_bound[...]
    forget_raw = owned(1)
    query_raw = owned(0)
    decay = bound + (1.0 - bound) * jax.nn.sigmoid(forget_raw)
    key_vec = (1.0 - bound) * jax.nn.sigmoid(-forget_raw)
    query_vec = jax.nn.silu(query_raw) * dim ** (-0.5)
    input_raw = owned(2)
    read_vec = query_vec * decay
    for h in range(heads):
        part = slice(h * dim, (h + 1) * dim)
        gates[h] = jnp.concatenate(
            [read_vec[:, part], decay[:, part], key_vec[:, part], input_raw[:, part]], axis=0
        )

    def read_step(h, carry):
        turned = gates[h].T
        out = [
            jnp.sum(turned[:, t : t + 1] * st[t, h], axis=0, keepdims=True) for t in range(rows)
        ]
        reads[h] = jnp.concatenate(out, axis=0)
        return carry

    lax.fori_loop(0, heads, read_step, 0, unroll=4)

    def update_step(h, carry):
        flat = gates[h]
        turned = flat.T
        for t in range(rows):
            st[t, h] = (
                turned[:, rows + t : rows + t + 1] * st[t, h]
                + turned[:, 2 * rows + t : 2 * rows + t + 1]
                * flat[3 * rows + t : 3 * rows + t + 1, :]
            )
        return carry

    gate_raw = owned(3)
    query_key = query_vec * key_vec
    mixed = jnp.concatenate(
        [
            rms_scale(
                reads[h]
                + jnp.sum(query_key[:, h * dim : (h + 1) * dim], axis=1, keepdims=True)
                * input_raw[:, h * dim : (h + 1) * dim],
                head_gain[...],
            )
            * jax.nn.silu(gate_raw[:, h * dim : (h + 1) * dim])
            for h in range(heads)
        ],
        axis=1,
    )
    mx_buf[me] = mixed.astype(BF16)

    copies = spread(2, mx_buf)
    loads[6].wait()
    pass_on(2, mx_buf, copies)

    def mixed_chunk(c, carry):
        x = jnp.concatenate([mx_buf[c * per + i].astype(F32) for i in range(per)], axis=0)
        r0 = pl.multiple_of(c * chunk, chunk)
        xn[pl.ds(r0, chunk), :] = x.astype(BF16)
        return carry

    lax.fori_loop(0, total // chunk, mixed_chunk, 0, unroll=2)
    col_buf[me] = jnp.dot(xn[...], wo[...], preferred_element_type=F32).astype(BF16)

    copies = spread(3, col_buf)
    pass_on(3, col_buf, copies)

    def middle_chunk(c, carry):
        r0 = pl.multiple_of(c * chunk, chunk)
        x = jnp.concatenate([tok_buf[c * per + i].astype(F32) for i in range(per)], axis=0)
        y = jnp.concatenate(
            [col_buf[s, pl.ds(r0, chunk), :].astype(F32) for s in range(n)], axis=1
        )
        middle = x + y
        for i in range(per):
            mid_buf[c * per + i] = middle[i * rows : (i + 1) * rows, :]
        xn[pl.ds(r0, chunk), :] = rms_scale(middle, norm_ffn[...]).astype(BF16)
        return carry

    lax.fori_loop(0, total // chunk, middle_chunk, 0, unroll=2)

    loads[7].wait()
    loads[8].wait()
    tile = 256 if hidden % 256 == 0 else hidden

    def up_tile(j, carry):
        part = pl.ds(pl.multiple_of(j * tile, tile) if tile % 128 == 0 else 0, tile)
        g = jnp.dot(xn[...], wg[:, part], preferred_element_type=F32)
        u = jnp.dot(xn[...], wu[:, part], preferred_element_type=F32)
        hid[:, part] = (jax.nn.silu(g) * u).astype(BF16)
        return carry

    lax.fori_loop(0, hidden // tile, up_tile, 0)
    loads[9].wait()
    out_tile = 256
    pieces = 2
    piece = width // pieces

    def down_tile(j, carry):
        part = pl.ds(pl.multiple_of(j * out_tile, out_tile), out_tile)
        d = jnp.dot(hid[...], wd[:, part], preferred_element_type=F32)
        for s in range(n):
            ps[s % 2, s // 2, :, part] = d[s * rows : (s + 1) * rows, :].astype(BF16)
        return carry

    per_piece = piece // out_tile
    halves = []
    for p in range(pieces):
        lax.fori_loop(p * per_piece, (p + 1) * per_piece, down_tile, 0, unroll=2)
        part = pl.ds(p * piece, piece)
        halves.append(
            send(4, p, ps.at[1 - core, :, :, part], fw.at[:, :, part], partner)
        )
    returns = []
    for p in range(pieces):
        part = pl.ds(p * piece, piece)
        halves[p].wait_recv()
        for c in range(chips):
            summed[c, :, part] = (
                ps[core, c, :, part].astype(F32) + fw[c, :, part].astype(F32)
            ).astype(BF16)
        for k in others:
            to = lax.rem(chip + k, chips)
            returns.append(
                send(
                    5 + p,
                    k,
                    summed.at[to, :, part],
                    ret_buf.at[chip, :, part],
                    away(k),
                )
            )
        ret_buf[chip, :, part] = summed[chip, :, part]
    lax.fori_loop(0, heads, update_step, 0, unroll=2)
    for copy in returns:
        copy.wait_recv()
    result = mid_buf[me]
    diagonal = lax.broadcasted_iota(jnp.int32, (rows, rows), 0) == lax.broadcasted_iota(
        jnp.int32, (rows, rows), 1
    )
    for e in range(EXPERTS):
        flat_share = jnp.sum(
            jnp.where(ids[...] == e, weights[...].astype(F32), 0.0), axis=0, keepdims=True
        )
        share = jnp.sum(jnp.where(diagonal, flat_share, 0.0), axis=1, keepdims=True)
        rows_e = ret_buf[e * group].astype(F32)
        for s in range(1, group):
            rows_e = rows_e + ret_buf[e * group + s].astype(F32)
        result = result + share * rows_e
    layer_out[...] = result.astype(BF16)

    for copy in sent:
        copy.wait_send()


def local(n, *args):
    (
        tokens,
        state,
        ids,
        weights,
        norm_mix,
        w_query,
        w_forget,
        w_input,
        w_gate,
        lower_bound,
        head_gain,
        w_out,
        norm_ffn,
        expert_gate,
        expert_up,
        expert_down,
    ) = args
    rows, width = tokens.shape
    heads, dim = state.shape[1], state.shape[2]
    cols = w_query.shape[1]
    hidden = expert_gate.shape[1]
    total = n * rows
    any_spec = pl.BlockSpec(memory_space=pltpu.HBM)
    vmem = pl.BlockSpec(memory_space=pltpu.VMEM)
    return pl.pallas_call(
        functools.partial(kernel, n),
        out_shape=(
            pltpu.VMEM(tokens.shape, tokens.dtype),
            pltpu.VMEM(state.shape, state.dtype),
        ),
        in_specs=[any_spec, any_spec, vmem, vmem] + [any_spec] * 12,
        out_specs=(vmem, vmem),
        scratch_shapes=[
            pltpu.VMEM((n, rows, width), BF16),
            pltpu.VMEM((1, width), F32),
            pltpu.VMEM((1, width), F32),
            pltpu.VMEM((1, dim), F32),
            pltpu.VMEM((1, width), F32),
            pltpu.VMEM((4, width, cols), BF16),
            pltpu.VMEM((width, cols), BF16),
            pltpu.VMEM((width, hidden), BF16),
            pltpu.VMEM((width, hidden), BF16),
            pltpu.VMEM((hidden, width), BF16),
            pltpu.VMEM((total, width), BF16),
            pltpu.VMEM((n, rows, 4 * cols), BF16),
            pltpu.VMEM((n, rows, 4 * cols), BF16),
            pltpu.VMEM((heads, 4 * rows, dim), F32),
            pltpu.VMEM((heads, rows, dim), F32),
            pltpu.VMEM((n, rows, width), BF16),
            pltpu.VMEM((n, total, cols), BF16),
            pltpu.VMEM((n, rows, width), F32),
            pltpu.VMEM((total, hidden), BF16),
            pltpu.VMEM((2, n // 2, rows, width), BF16),
            pltpu.VMEM((n // 2, rows, width), BF16),
            pltpu.VMEM((n // 2, rows, width), BF16),
            pltpu.VMEM((n // 2, rows, width), BF16),
            pltpu.SemaphoreType.DMA((14,)),
            pltpu.SemaphoreType.DMA((7, n)),
            pltpu.SemaphoreType.DMA((7, n)),
        ],
        compiler_params=pltpu.CompilerParams(
            collective_id=0,
            has_side_effects=True,
            vmem_limit_bytes=VMEM - 4 * state.size - 64 * 1024,
        ),
    )(
        tokens,
        state,
        ids.T,
        weights.T,
        norm_mix[None],
        w_query,
        w_forget,
        w_input,
        w_gate,
        lower_bound[None],
        head_gain[None],
        w_out,
        norm_ffn[None],
        expert_gate,
        expert_up,
        expert_down,
    )


def solution(mesh):
    return jax.shard_map(
        functools.partial(local, mesh.shape["ep"]),
        mesh=mesh,
        in_specs=(
            P(("grp", "ep"), None),
            P(("grp", "ep"), None, None, None),
            P(("grp", "ep"), None),
            P(("grp", "ep"), None),
            P(),
            P(None, "ep"),
            P(None, "ep"),
            P(None, "ep"),
            P(None, "ep"),
            P(),
            P(),
            P(None, "ep"),
            P(),
            P(None, "ep"),
            P(None, "ep"),
            P("ep", None),
        ),
        out_specs=(P(("grp", "ep"), None), P(("grp", "ep"), None, None, None)),
        check_vma=False,
    )
```
